32 devices in a mesh: ep: 8 (over z, x), tp: 4 (over y, core).
Axes of the slice: x: 2, y: 2, z: 4, core: 2. Of those that a mesh axis runs over, the one named last changes fastest.
Arguments:
- tokens: bfloat16 [32, 2048], P('ep'), may hold values from -6 to 6
- attn_gain: bfloat16 [2048], replicated, may hold values from 0.099609375 to 1.8984375
- ffn_gain: bfloat16 [2048], replicated, may hold values from 0.099609375 to 1.8984375
- w_query: bfloat16 [2048, 2048], P(None, 'tp'), may hold values from -0.125 to 0.125
- w_key: bfloat16 [2048, 256], replicated, may hold values from -0.125 to 0.125
- w_value: bfloat16 [2048, 256], replicated, may hold values from -0.125 to 0.125
- w_forget: bfloat16 [2048, 32], replicated, may hold values from -0.125 to 0.125
- forget_bias: float32 [32], replicated, may hold values from -1 to 3
- w_out: bfloat16 [2048, 2048], P(None, 'tp'), may hold values from -0.375 to 0.375
- cache_keys: bfloat16 [32, 2048, 256], P(('ep', 'tp')), may hold values from -800 to 800
- cache_values: bfloat16 [32, 2048, 256], P(('ep', 'tp')), may hold values from -6 to 6
- cache_logcum: float32 [32, 32, 2048], P(('ep', 'tp')), as said below
- cache_len: int32 [32], P(('ep', 'tp')), may hold values from 256 to 2048
- route_group: int32 [32], P('ep'), may hold values from 0 to 3, as said below
- route_expert: int32 [32, 2], P('ep'), may hold values from 0 to 1, as said below
- route_weight: float32 [32, 2], P('ep'), may hold values from 0.2 to 1
- w_gate: bfloat16 [8, 2048, 2048], P('ep', None, 'tp'), may hold values from -0.125 to 0.125
- w_up: bfloat16 [8, 2048, 2048], P('ep', None, 'tp'), may hold values from -0.125 to 0.125
- w_down: bfloat16 [8, 2048, 2048], P('ep', None, 'tp'), may hold values from -0.125 to 0.125
Outputs:
- layer_out: bfloat16 [32, 2048], P('ep', 'tp')
The draws below stay inside these ranges and needn't reach their ends.
Inputs may be any that keep to these rules, and one draw needn't show every extreme that they name: Expert groups. Among the 4 sequences of one index of ep no expert route_group * 2 + route_expert is named more than 3 times, and in every draw one expert is named exactly 3 times by the sequences of every index of ep. `route_expert`: the 2 numbers of a sequence differ. `cache_logcum`: each entry is the sum of the log forget gates of that head from the first cached position up to and including that position.
All inputs are finite; a program needn't handle non-finite values.
Results may differ from the reference program's by a relative error of at most 0.012.
The reference program's roundings to bfloat16 on the way count: a program that leaves them out, or rounds other values in their place, can miss the bound.
Values may be sent and summed in bfloat16 or wider, within the bound.
A program may use at most 64 MiB of HBM per device.

```python
import math
import jax
import jax.numpy as jnp
from jax import lax

D = 2048
QUERY_HEAD_COUNT = 32
KV_HEADS = 4
HEAD = 64
FE = 2048
GROUPS = 4
TOP = 2
CACHE_LENGTH = 2048
GROUP_SEQS = 4
SEQUENCE_TOTAL = 32
EXPERTS = 8
CAP = 3
N_EP = 8


def draw_cache_keys(key, part):
    random_subkeys = jax.random.split(jax.random.fold_in(key, 3), 1)
    base_keys = jnp.clip(jax.random.normal(random_subkeys[0], (SEQUENCE_TOTAL, CACHE_LENGTH, KV_HEADS * HEAD), jnp.float32), -6.0, 6.0)
    return base_keys.astype(jnp.bfloat16)


def draw_cache_logcum(key, part):
    random_subkeys = jax.random.split(jax.random.fold_in(key, 5), 8)
    slow_heads = jax.random.bernoulli(random_subkeys[0], 0.5, (QUERY_HEAD_COUNT,))
    jitter = jnp.exp(jax.random.uniform(random_subkeys[6], (SEQUENCE_TOTAL, QUERY_HEAD_COUNT, CACHE_LENGTH), jnp.float32, math.log(0.3), math.log(3.0)))
    slow_rate = jnp.exp(jax.random.uniform(random_subkeys[1], (QUERY_HEAD_COUNT,), jnp.float32, math.log(0.2), math.log(0.6))) / CACHE_LENGTH
    fast_rate = 1.0 / jnp.exp(jax.random.uniform(random_subkeys[2], (QUERY_HEAD_COUNT,), jnp.float32, math.log(30.0), math.log(100.0)))
    decay_rate = jnp.where(slow_heads, slow_rate, fast_rate)
    seq_factor = jnp.exp(jax.random.uniform(random_subkeys[3], (SEQUENCE_TOTAL, 1, 1), jnp.float32, math.log(0.5), math.log(2.0)))
    block_factor = jnp.exp(jax.random.uniform(random_subkeys[4], (SEQUENCE_TOTAL, 1, 16), jnp.float32, math.log(0.7), math.log(1.4)))
    cache_position = jnp.arange(CACHE_LENGTH)
    block_index = cache_position * 16 // CACHE_LENGTH
    block_scale = block_factor[:, :, block_index]
    step_increments = -decay_rate[None, :, None] * seq_factor * block_scale * jitter
    spike_events = jax.random.randint(random_subkeys[5], (SEQUENCE_TOTAL, 3), 0, CACHE_LENGTH)
    spike_penalty = jnp.log(jax.random.uniform(random_subkeys[7], (SEQUENCE_TOTAL, 3), jnp.float32, 0.5, 0.8))
    match_counts = (cache_position[None, None, :] == spike_events[:, :, None]).astype(jnp.float32)
    step_increments = step_increments + jnp.sum(match_counts * spike_penalty[:, :, None], axis=1)[:, None, :]
    return jnp.cumsum(step_increments, axis=-1)


def routing_draw(key):
    random_subkeys = jax.random.split(key, 6)
    per_group = EXPERTS // GROUPS
    heavy_group = jax.random.randint(random_subkeys[0], (), 0, GROUPS)
    heavy_perm = jax.random.permutation(random_subkeys[1], per_group)
    fewest_rows = per_group * (CAP - 1) // TOP + 1
    heavy_rows = min(per_group * CAP // TOP, GROUP_SEQS)
    heavy_count = jax.random.randint(random_subkeys[2], (N_EP, 1), fewest_rows, heavy_rows + 1)
    row_order = jax.vmap(lambda subkey: jax.random.permutation(subkey, GROUP_SEQS))(jax.random.split(random_subkeys[3], N_EP))
    other_group = (heavy_group + 1 + jax.random.randint(random_subkeys[4], (N_EP, GROUP_SEQS), 0, GROUPS - 1)) % GROUPS
    group_ids = jnp.where(row_order < heavy_count, heavy_group, other_group)
    same_group = group_ids[:, :, None] == group_ids[:, None, :]
    earlier = row_order[:, None, :] < row_order[:, :, None]
    rank_in_group = jnp.sum((same_group & earlier).astype(jnp.int32), axis=2)
    group_perms = jax.vmap(lambda subkey: jax.random.permutation(subkey, per_group))(jax.random.split(random_subkeys[5], N_EP * GROUPS))
    group_perms = group_perms.reshape(N_EP, GROUPS, per_group)
    group_perms = jnp.where(jnp.arange(GROUPS)[None, :, None] == heavy_group, heavy_perm[None, None, :], group_perms)
    row_table = jnp.take_along_axis(group_perms, group_ids[:, :, None], axis=1)
    picks = []
    for choice_index in range(TOP):
        slot_index = (TOP * rank_in_group + choice_index) % per_group
        picks.append(jnp.take_along_axis(row_table, slot_index[:, :, None], axis=2)[:, :, 0])
    experts_local = jnp.stack(picks, axis=-1)
    return (group_ids.reshape(SEQUENCE_TOTAL).astype(jnp.int32), experts_local.reshape(SEQUENCE_TOTAL, TOP).astype(jnp.int32))


def draw_route_group(key, part):
    return routing_draw(jax.random.fold_in(key, 17))[0]


def draw_route_expert(key, part):
    return routing_draw(jax.random.fold_in(key, 17))[1]


def place_ends(values, key, low, largest):
    longest = values.shape.index(max(values.shape))
    spots = []
    for shift in (0, 1):
        where = [jax.random.randint(jax.random.fold_in(key, axis), (), 0, length) for axis, length in enumerate(values.shape)]
        where[longest] = (where[longest] + shift) % values.shape[longest]
        spots.append(tuple(where))
    return values.at[spots[0]].set(low).at[spots[1]].set(largest)


def level_of(rng, extent, cuts, least, largest):
    factor_of = 1.0
    for dim, blocks in cuts:
        steps = jax.random.uniform(jax.random.fold_in(jax.random.fold_in(rng, 6), dim), (blocks,), jnp.float32, least / len(cuts), largest / len(cuts))
        factor_of = factor_of * jnp.repeat(jnp.exp(steps), extent[dim] // blocks).reshape((-1,) + (1,) * (len(extent) - 1 - dim))
    return factor_of


def centred(key, shape, scale, limit, cuts=(), kind=jnp.bfloat16):
    drawn = scale * jax.random.normal(key, shape, jnp.float32)
    if cuts:
        drawn = drawn * level_of(key, shape, cuts, -0.22, 0.18)
    return jnp.clip(drawn, -limit, limit).astype(kind)


def setup_inputs(seed: int = 0) -> dict:
    streams_of = jax.random.split(jax.random.key(seed), 20)
    tokens = centred(streams_of[0], (SEQUENCE_TOTAL, D), 1.0, 6.0, ((0, 8),))
    attn_gain = jnp.clip(1.0 + 0.18 * jax.random.normal(streams_of[1], (D,), jnp.float32), 0.099609375, 1.8984375).astype(jnp.bfloat16)
    ffn_gain = jnp.clip(1.0 + 0.18 * jax.random.normal(streams_of[2], (D,), jnp.float32), 0.099609375, 1.8984375).astype(jnp.bfloat16)
    w_query = centred(streams_of[3], (D, QUERY_HEAD_COUNT * HEAD), D ** -0.5, 0.125, ((1, 4),))
    w_key = centred(streams_of[4], (D, KV_HEADS * HEAD), D ** -0.5, 0.125)
    w_value = centred(streams_of[5], (D, KV_HEADS * HEAD), D ** -0.5, 0.125)
    w_forget = centred(streams_of[6], (D, QUERY_HEAD_COUNT), D ** -0.5, 0.125)
    forget_bias = jnp.clip(jax.random.uniform(streams_of[7], (QUERY_HEAD_COUNT,), jnp.float32, -1.0, 3.0), -1.0, 3.0)
    w_out = centred(streams_of[8], (QUERY_HEAD_COUNT * HEAD, D), (QUERY_HEAD_COUNT * HEAD // 8) ** -0.5, 0.375, ((1, 4),))
    cache_keys = draw_cache_keys(jax.random.fold_in(streams_of[19], 71), 0)
    cache_values = centred(streams_of[10], (SEQUENCE_TOTAL, CACHE_LENGTH, KV_HEADS * HEAD), 1.0, 6.0, ((0, 32),))
    cache_logcum = draw_cache_logcum(jax.random.fold_in(streams_of[19], 71), 0)
    cache_len = place_ends(jax.random.randint(streams_of[12], (SEQUENCE_TOTAL,), CACHE_LENGTH // 8, CACHE_LENGTH + 1), jax.random.fold_in(streams_of[12], 1), CACHE_LENGTH // 8, CACHE_LENGTH).astype(jnp.int32)
    route_group = draw_route_group(jax.random.fold_in(streams_of[19], 71), 0)
    route_expert = draw_route_expert(jax.random.fold_in(streams_of[19], 71), 0)
    route_weight = jnp.clip(jnp.exp(math.log(1.0) - 1.609438 * jax.random.uniform(streams_of[15], (SEQUENCE_TOTAL, TOP), jnp.float32) ** level_of(streams_of[15], (SEQUENCE_TOTAL, TOP), ((0, 8),), -0.2, 0.2)), 0.2, 1.0)
    w_gate = centred(streams_of[16], (EXPERTS, D, FE), D ** -0.5, 0.125, ((0, 8), (2, 4)))
    w_up = centred(streams_of[17], (EXPERTS, D, FE), D ** -0.5, 0.125, ((0, 8), (2, 4)))
    w_down = centred(streams_of[18], (EXPERTS, FE, D), FE ** -0.5, 0.125, ((0, 8), (2, 4)))
    return dict(tokens=tokens, attn_gain=attn_gain, ffn_gain=ffn_gain, w_query=w_query, w_key=w_key, w_value=w_value, w_forget=w_forget, forget_bias=forget_bias, w_out=w_out, cache_keys=cache_keys, cache_values=cache_values, cache_logcum=cache_logcum, cache_len=cache_len, route_group=route_group, route_expert=route_expert, route_weight=route_weight, w_gate=w_gate, w_up=w_up, w_down=w_down)


NORM_EPSILON = 1e-06
MASKED_SCORE = -1e+30

def normalize(values, gain_vec):
    return values * lax.rsqrt(lax.optimization_barrier(jnp.mean(values * values, axis=-1, keepdims=True)) + NORM_EPSILON) * gain_vec.astype(jnp.float32)

def attend_block(arguments):
    query, key_new, value_new, log_gate, keys, cached_values, logcum, lengths = arguments
    count_of_rows = query.shape[0]
    length = keys.shape[1]
    per_kv = QUERY_HEAD_COUNT // KV_HEADS
    score_scale = HEAD ** (-0.5)
    query_float = query.astype(jnp.float32).reshape(count_of_rows, KV_HEADS, per_kv, HEAD)
    keys_f = keys.astype(jnp.float32).reshape(count_of_rows, length, KV_HEADS, HEAD)
    scores = jnp.einsum('bkgd,blkd->bkgl', query_float, keys_f).reshape(count_of_rows, QUERY_HEAD_COUNT, length) * score_scale
    latest = jnp.take_along_axis(logcum, (lengths - 1).astype(jnp.int32)[:, None, None], axis=2)
    scores = scores + latest + log_gate[:, :, None] - logcum
    usable = jnp.arange(length, dtype=jnp.int32)[None, None, :] < lengths[:, None, None]
    scores = jnp.where(usable, scores, MASKED_SCORE)
    current_key = key_new.astype(jnp.float32).reshape(count_of_rows, KV_HEADS, HEAD)
    current_score = jnp.einsum('cnpx,cnx->cnp', query_float, current_key).reshape(count_of_rows, QUERY_HEAD_COUNT) * score_scale
    peak = jnp.maximum(lax.optimization_barrier(jnp.max(scores, axis=2)), current_score)
    weights = jnp.where(usable, jnp.exp(scores - peak[:, :, None]), 0.0)
    own_weight = jnp.exp(current_score - peak)
    denominator = lax.optimization_barrier(jnp.sum(weights, axis=2)) + own_weight
    weights_b = lax.optimization_barrier(weights.astype(jnp.bfloat16)).astype(jnp.float32)
    own_b = lax.optimization_barrier(own_weight.astype(jnp.bfloat16)).astype(jnp.float32)
    values_f = cached_values.astype(jnp.float32).reshape(count_of_rows, length, KV_HEADS, HEAD)
    summed = jnp.einsum('bkgl,blkd->bkgd', weights_b.reshape(count_of_rows, KV_HEADS, per_kv, length), values_f)
    own_value = value_new.astype(jnp.float32).reshape(count_of_rows, KV_HEADS, 1, HEAD)
    summed = summed + own_b.reshape(count_of_rows, KV_HEADS, per_kv)[..., None] * own_value
    summed = summed.reshape(count_of_rows, QUERY_HEAD_COUNT, HEAD) / denominator[:, :, None]
    return summed.reshape(count_of_rows, QUERY_HEAD_COUNT * HEAD).astype(jnp.bfloat16)

def reference(tokens, attn_gain, ffn_gain, w_query, w_key, w_value, w_forget, forget_bias, w_out, cache_keys, cache_values, cache_logcum, cache_len, route_group, route_expert, route_weight, w_gate, w_up, w_down):
    stream = tokens.astype(jnp.float32)
    normed = normalize(stream, attn_gain).astype(jnp.bfloat16)
    query = jnp.dot(normed, w_query, preferred_element_type=jnp.float32).astype(jnp.bfloat16)
    key_new = jnp.dot(normed, w_key, preferred_element_type=jnp.float32).astype(jnp.bfloat16)
    value_new = jnp.dot(normed, w_value, preferred_element_type=jnp.float32).astype(jnp.bfloat16)
    log_gate = jax.nn.log_sigmoid(jnp.dot(normed, w_forget, preferred_element_type=jnp.float32) + forget_bias.astype(jnp.float32))

    def by_group(array):
        return array.reshape((N_EP, GROUP_SEQS) + array.shape[1:])
    pieces = tuple((by_group(array) for array in (query, key_new, value_new, log_gate, cache_keys, cache_values, cache_logcum, cache_len)))
    attended = lax.map(attend_block, pieces).reshape(SEQUENCE_TOTAL, QUERY_HEAD_COUNT * HEAD)
    mixed = (stream + jnp.dot(attended, w_out, preferred_element_type=jnp.float32)).astype(jnp.bfloat16)
    inputs = normalize(mixed.astype(jnp.float32), ffn_gain).astype(jnp.bfloat16)
    experts_per_group = EXPERTS // GROUPS
    picked_ids = (route_group[:, None] * experts_per_group + route_expert).reshape(-1).astype(jnp.int32)
    max_rows = N_EP * CAP
    pick_count = SEQUENCE_TOTAL * TOP

    def one_expert(collected, expert_item):
        gate_weight, up_weight, down_weight, expert_index = expert_item
        chosen = jnp.nonzero(picked_ids == expert_index, size=max_rows, fill_value=pick_count)[0]
        row_data = inputs[jnp.minimum(chosen, pick_count - 1) // TOP]
        gate_proj = jnp.dot(row_data, gate_weight, preferred_element_type=jnp.float32)
        up_proj = jnp.dot(row_data, up_weight, preferred_element_type=jnp.float32)
        hidden = (jax.nn.silu(gate_proj) * up_proj).astype(jnp.bfloat16)
        result = jnp.dot(hidden, down_weight, preferred_element_type=jnp.float32).astype(jnp.bfloat16)
        result = lax.optimization_barrier(result).astype(jnp.float32)
        return (collected.at[chosen].set(result, mode='drop'), None)
    expert_order = jnp.arange(EXPERTS, dtype=jnp.int32)
    picked, _ = lax.scan(one_expert, jnp.zeros((pick_count, D), jnp.float32), (w_gate, w_up, w_down, expert_order))
    moe_sum = lax.optimization_barrier(jnp.sum(route_weight.astype(jnp.float32)[:, :, None] * picked.reshape(SEQUENCE_TOTAL, TOP, D), axis=1))
    return (mixed.astype(jnp.float32) + moe_sum).astype(jnp.bfloat16)
```

```python
import functools

import jax
import jax.numpy as jnp
from jax import lax
from jax.experimental import pallas as pl
from jax.experimental.pallas import tpu as pltpu
from jax.sharding import PartitionSpec as P

QUERY_HEAD_COUNT = 32
KV_HEADS = 4
HEAD = 64
GROUPS = 4
TOP = 2
PER_KV = QUERY_HEAD_COUNT // KV_HEADS
LANES = 128
Q_PARTS = 4
NORM_EPSILON = 1e-06
MASKED_SCORE = -1e30
F32 = jnp.float32
BF16 = jnp.bfloat16
MESH = pl.DeviceIdType.MESH


def dot(a, b):
    return jnp.dot(a, b, preferred_element_type=F32)


def as_row(ref):
    block = ref[...].astype(F32)
    return jnp.concatenate([block[i : i + 1] for i in range(block.shape[0])], axis=1)


def each(count, body):
    if count <= 8:
        for step in range(count):
            body(step)
    else:

        @pl.loop(0, count)
        def _(step):
            body(step)


def kernel(
    n_ep,
    n_tp,
    tokens_hbm,
    attn_gain_hbm,
    ffn_gain_hbm,
    forget_bias_hbm,
    cache_len_hbm,
    route_group_hbm,
    route_expert_hbm,
    route_weight_hbm,
    wq_hbm,
    wk_hbm,
    wv_hbm,
    wf_hbm,
    wo_hbm,
    keys_hbm,
    values_hbm,
    logcum_hbm,
    wg_hbm,
    wu_hbm,
    wd_hbm,
    out,
    tokens,
    attn_gain,
    ffn_gain,
    forget_bias,
    cache_len,
    route_group,
    route_expert,
    route_weight,
    wq,
    wk,
    wv,
    wf,
    wo,
    keys,
    values,
    logcum,
    wg,
    wu,
    wd,
    q_send,
    q_recv,
    att_send,
    att_recv,
    att_rows,
    mix_send,
    mix_recv,
    hid_send,
    hid_recv,
    ret_send,
    ret_recv,
    load_sem,
    q_ssem,
    q_rsem,
    att_ssem,
    att_rsem,
    mix_ssem,
    mix_rsem,
    relay_ssem,
    hid_ssem,
    hid_rsem,
    ret_ssem,
    ret_rsem,
    near_sem,
    gain_parts,
):
    ep = lax.axis_index("ep")
    tp = lax.axis_index("tp")
    pairs = n_tp // 2

    def tp_peer(offset):
        pair = lax.rem(tp // 2 + offset // 2, pairs)
        core = lax.rem(lax.rem(tp, 2) + offset % 2, 2)
        return pair * 2 + core

    def tp_source(offset):
        pair = lax.rem(tp // 2 + pairs - offset // 2, pairs)
        core = lax.rem(lax.rem(tp, 2) + offset % 2, 2)
        return pair * 2 + core

    def ep_peer(offset):
        return lax.rem(ep + offset, n_ep)

    def far_first(step, skip):
        return skip + lax.rem(step + n_ep // 2 - 2 * skip, n_ep - skip)

    q_part = wq.shape[0] // Q_PARTS
    q_names = [f"wq{i}" for i in range(Q_PARTS)]
    loads = {}
    for index, (name, source, target) in enumerate(
        (
            ("tokens", tokens_hbm, tokens),
            ("attn_gain", attn_gain_hbm, attn_gain),
            ("ffn_gain", ffn_gain_hbm, ffn_gain),
            ("forget_bias", forget_bias_hbm, forget_bias),
            ("cache_len", cache_len_hbm, cache_len),
            ("route_group", route_group_hbm, route_group),
            ("route_expert", route_expert_hbm, route_expert),
            ("route_weight", route_weight_hbm, route_weight),
            *[
                (f"wq{i}", wq_hbm.at[pl.ds(i * q_part, q_part)], wq.at[pl.ds(i * q_part, q_part)])
                for i in range(Q_PARTS)
            ],
            ("wk", wk_hbm, wk),
            ("wv", wv_hbm, wv),
            ("wf", wf_hbm, wf),
            ("logcum", logcum_hbm.at[0], logcum),
            ("keys", keys_hbm.at[0], keys),
            ("values", values_hbm.at[0], values),
            ("wo", wo_hbm, wo),
            ("wg", wg_hbm.at[0], wg),
            ("wu", wu_hbm.at[0], wu),
            ("wd", wd_hbm.at[0], wd),
        )
    ):
        loads[name] = pltpu.make_async_copy(source, target, load_sem.at[index])
    small = ("ffn_gain", "forget_bias", "cache_len", "route_group", "route_expert", "route_weight")
    for name in ("tokens", "attn_gain", *q_names):
        loads[name].start()

    barrier = pltpu.get_barrier_semaphore()
    leader = n_tp - 1
    for offset in range(1, n_tp):
        pl.semaphore_signal(barrier, inc=1, device_id=(ep, tp_peer(offset)), device_id_type=MESH)
    for name in ("wk", "wv", "wf", *small, "logcum", "keys", "values", "wo", "wg", "wu", "wd"):
        loads[name].start()

    rows = tokens.shape[0]
    width = wo.shape[1]
    depth = tokens.shape[1]
    length = keys.shape[0]
    loads["tokens"].wait()
    loads["attn_gain"].wait()
    stream = tokens[...].astype(F32)
    square = jnp.mean(stream * stream, axis=-1, keepdims=True)
    normed = (stream * lax.rsqrt(square + NORM_EPSILON) * as_row(attn_gain)).astype(BF16)

    query = None
    for i, name in enumerate(q_names):
        loads[name].wait()
        term = dot(normed[:, i * q_part : (i + 1) * q_part], wq[i * q_part : (i + 1) * q_part, :])
        query = term if query is None else query + term
    query = query.astype(BF16).astype(F32)
    for row in range(rows):
        q_send[row] = query[row : row + 1, :]

    @pl.when(tp != leader)
    def _():
        pl.semaphore_wait(barrier, n_tp - 1)
        pl.semaphore_signal(near_sem.at[0], inc=1, device_id=(ep, leader), device_id_type=MESH)

    @pl.when(tp == leader)
    def _():
        pl.semaphore_wait(near_sem.at[0], n_tp - 1)

        def announce(step):
            pl.semaphore_signal(
                barrier, inc=1, device_id=(ep_peer(step + 1), leader), device_id_type=MESH
            )

        each(n_ep - 1, announce)

    def q_copy(offset):
        peer = tp_peer(offset)
        return pltpu.make_async_remote_copy(
            src_ref=q_send.at[peer],
            dst_ref=q_recv.at[tp],
            send_sem=q_ssem.at[offset],
            recv_sem=q_rsem.at[offset],
            device_id=(ep, peer),
            device_id_type=MESH,
        )

    q_copies = [q_copy(offset) for offset in range(1, n_tp)]
    for copy in q_copies:
        copy.start()
    q_recv[tp] = q_send[tp]

    own = lax.broadcasted_iota(jnp.int32, (rows, 1), 0) == tp

    def own_row(values_all):
        return jnp.sum(jnp.where(own, values_all, 0.0), axis=0, keepdims=True)

    loads["wk"].wait()
    key_new = own_row(dot(normed, wk[...])).astype(BF16).astype(F32)
    loads["wv"].wait()
    value_new = own_row(dot(normed, wv[...])).astype(BF16).astype(F32)
    loads["wf"].wait()
    for name in small:
        loads[name].wait()
    heads = QUERY_HEAD_COUNT
    gates = lax.dot_general(
        wf[...], normed, (((1,), (1,)), ((), ())), preferred_element_type=F32
    )
    own_lane = lax.broadcasted_iota(jnp.int32, (1, rows), 1) == tp
    gate_sum = jnp.sum(jnp.where(own_lane, gates, 0.0), axis=1, keepdims=True)
    diagonal = lax.broadcasted_iota(jnp.int32, (heads, heads), 0) == lax.broadcasted_iota(
        jnp.int32, (heads, heads), 1
    )
    bias_sum = jnp.sum(jnp.where(diagonal, forget_bias[...], 0.0), axis=1, keepdims=True)
    log_gate = jax.nn.log_sigmoid(gate_sum + bias_sum)
    used = cache_len[0, 0]
    position = lax.broadcasted_iota(jnp.int32, (1, length), 1)
    loads["logcum"].wait()
    cum = logcum[...]
    latest = jnp.sum(jnp.where(position == used - 1, cum, 0.0), axis=1, keepdims=True)
    bias = jnp.where(position < used, (latest + log_gate) - cum, MASKED_SCORE)

    loads["keys"].wait()
    for copy in q_copies:
        copy.wait_recv()

    span = PER_KV * HEAD
    q_row = jnp.concatenate([q_recv[source] for source in range(n_tp)], axis=1)
    row_of = lax.broadcasted_iota(jnp.int32, (PER_KV, span), 0)
    lane_of = lax.broadcasted_iota(jnp.int32, (PER_KV, span), 1) // HEAD
    half_of = lax.broadcasted_iota(jnp.int32, (PER_KV, LANES), 1) // HEAD
    zeros = jnp.zeros((PER_KV, LANES), F32)
    blocks = []
    for head in range(KV_HEADS):
        part = jnp.broadcast_to(q_row[:, head * span : (head + 1) * span], (PER_KV, span))
        part = jnp.where(row_of == lane_of, part, 0.0)
        fold = part[:, :LANES]
        for tile in range(1, span // LANES):
            fold = fold + part[:, tile * LANES : (tile + 1) * LANES]
        fold = fold + pltpu.roll(fold, HEAD, 1)
        fold = jnp.where(half_of == head % 2, fold, 0.0)
        tiles = [zeros] * (KV_HEADS * HEAD // LANES)
        tiles[head * HEAD // LANES] = fold
        blocks.append(jnp.concatenate(tiles, axis=1))
    q_heads = jnp.concatenate(blocks, axis=0)
    scale = HEAD ** (-0.5)
    own_score = jnp.sum(q_heads * key_new, axis=1, keepdims=True) * scale
    score = lax.dot_general(
        q_heads.astype(BF16), keys[...], (((1,), (1,)), ((), ())), preferred_element_type=F32
    )
    score = score * scale + bias
    peak = jnp.maximum(jnp.max(score, axis=1, keepdims=True), own_score)
    weight = jnp.exp(score - peak)
    own_weight = jnp.exp(own_score - peak)
    denominator = jnp.sum(weight, axis=1, keepdims=True) + own_weight
    loads["values"].wait()
    summed = dot(weight.astype(BF16), values[...])
    summed = summed + own_weight.astype(BF16).astype(F32) * value_new
    summed = summed / denominator
    kv_of = lax.broadcasted_iota(jnp.int32, (PER_KV, KV_HEADS * HEAD), 1) // HEAD
    folded = summed[:PER_KV]
    for head in range(1, KV_HEADS):
        folded = jnp.where(kv_of == head, summed[head * PER_KV : (head + 1) * PER_KV], folded)
    attended = folded.astype(BF16)
    att_send[...] = attended

    def att_copy(offset):
        return pltpu.make_async_remote_copy(
            src_ref=att_send,
            dst_ref=att_recv.at[tp],
            send_sem=att_ssem.at[offset],
            recv_sem=att_rsem.at[offset],
            device_id=(ep, tp_peer(offset)),
            device_id_type=MESH,
        )

    att_copies = [att_copy(offset) for offset in range(1, n_tp)]
    for copy in att_copies[::-1]:
        copy.start()
    att_recv[tp] = attended
    loads["wo"].wait()

    @pl.when(tp == leader)
    def _():
        pl.semaphore_wait(barrier, n_tp + n_ep - 2)
        for offset in range(1, n_tp):
            pl.semaphore_signal(
                near_sem.at[1], inc=1, device_id=(ep, tp_peer(offset)), device_id_type=MESH
            )

    gain = as_row(ffn_gain)
    for source in range(n_tp):
        gain_parts[source] = gain[:, source * width : (source + 1) * width]
    for copy in att_copies:
        copy.wait_recv()
    for source in range(n_tp):
        arrived = att_recv[source].astype(F32)
        for tile in range(att_rows.shape[0]):
            att_rows[tile, source * PER_KV : (source + 1) * PER_KV] = arrived[
                :, tile * LANES : (tile + 1) * LANES
            ]
    left = jnp.concatenate(
        [
            att_rows[tile, pl.ds(j, n_tp, stride=PER_KV), :]
            for j in range(PER_KV)
            for tile in range(att_rows.shape[0])
        ],
        axis=1,
    ).astype(BF16)
    right = jnp.concatenate(
        [
            wo[head * span + j * HEAD : head * span + (j + 1) * HEAD, :]
            for j in range(PER_KV)
            for head in range(KV_HEADS)
        ],
        axis=0,
    )
    projected = dot(left, right)
    residual = tokens[:, pl.ds(pl.multiple_of(tp * width, LANES), width)].astype(F32)
    mixed = (residual + projected).astype(BF16)
    mix_send[...] = mixed

    @pl.when(tp != leader)
    def _():
        pl.semaphore_wait(near_sem.at[1], 1)

    core = lax.rem(tp, 2)
    batches = hid_send.shape[0]
    span_ep = n_ep // batches
    batch = ep // span_ep

    def mix_copy(step, y_off, sem):
        return pltpu.make_async_remote_copy(
            src_ref=mix_send,
            dst_ref=mix_recv.at[tp, ep],
            send_sem=mix_ssem.at[sem],
            recv_sem=mix_rsem.at[tp, batch],
            device_id=(ep_peer(step), lax.rem(tp // 2 + y_off, pairs) * 2 + 1),
            device_id_type=MESH,
        )

    for y_off in range(pairs - 1, -1, -1):
        each(n_ep - 1, lambda step, y_off=y_off: mix_copy(far_first(step, 1), y_off, y_off).start())
    near_copies = [mix_copy(0, y_off, pairs + y_off) for y_off in range(pairs)]
    for copy in near_copies[1:]:
        copy.start()

    @pl.when(core == 0)
    def _():
        near_copies[0].start()

    @pl.when(core == 1)
    def _():
        pltpu.make_async_copy(mix_send, mix_recv.at[tp, ep], mix_rsem.at[tp, batch]).start()

    def mix_source(k):
        return lax.rem(tp // 2 + k % pairs, pairs) * 2 + (1 if k < pairs else 0)

    def mix_block(k, b):
        return mix_recv.at[mix_source(k), pl.ds(b * span_ep, span_ep)]

    def mix_wait(k, b):
        block = mix_block(k, b)
        pltpu.make_async_copy(block, block, mix_rsem.at[mix_source(k), b]).wait()

    def relay_copy(k, b):
        block = mix_block(k, b)
        return pltpu.make_async_remote_copy(
            src_ref=block,
            dst_ref=block,
            send_sem=relay_ssem.at[k, b],
            recv_sem=mix_rsem.at[mix_source(k), b],
            device_id=(ep, tp - core),
            device_id_type=MESH,
        )

    chunks, _, chunk = hid_send.shape[1:]
    hid_copies = {}

    def expand(b):
        gates, ups = [None] * chunks, [None] * chunks
        square = None

        @pl.when(core == 1)
        def _():
            for k in range(n_tp):
                mix_wait(k, b)
                relay_copy(k, b).start()

        for k in range(n_tp):
            @pl.when(core == 0)
            def _(k=k):
                mix_wait(k, b)

            if b == 0 and k == 0:
                loads["wg"].wait()
                loads["wu"].wait()
            source = mix_source(k)
            wide = jnp.concatenate(
                [mix_recv[source, b * span_ep + e].astype(F32) for e in range(span_ep)], axis=0
            )
            term = jnp.sum(wide * wide, axis=-1, keepdims=True)
            square = term if square is None else square + term
            scaled = (wide * gain_parts[source]).astype(BF16)
            start = pl.multiple_of(source * width, LANES)
            for c in range(chunks):
                cols = slice(c * chunk, (c + 1) * chunk)
                gate = dot(scaled, wg[pl.ds(start, width), cols])
                up = dot(scaled, wu[pl.ds(start, width), cols])
                gates[c] = gate if k == 0 else gates[c] + gate
                ups[c] = up if k == 0 else ups[c] + up
        factor = lax.rsqrt(square * (1.0 / depth) + NORM_EPSILON)
        for c in range(chunks):
            gate = gates[c] * factor
            hidden = (gate / (1.0 + jnp.exp(-gate)) * (ups[c] * factor)).astype(BF16)
            hid_send[b, c] = hidden
            for offset in range(n_tp - 1, 0, -1):
                hid_copies[b, c, offset] = pltpu.make_async_remote_copy(
                    src_ref=hid_send.at[b, c],
                    dst_ref=hid_recv.at[tp, b, c],
                    send_sem=hid_ssem.at[b, c, offset],
                    recv_sem=hid_rsem.at[b, c, offset],
                    device_id=(ep, tp_peer(offset)),
                    device_id_type=MESH,
                )
                hid_copies[b, c, offset].start()

    def ret_copy(b, step):
        peer = b * span_ep + lax.rem(ep + span_ep // 2 + step, span_ep)

        @pl.when(peer != ep)
        def _():
            pltpu.make_async_remote_copy(
                src_ref=ret_send.at[peer],
                dst_ref=ret_recv.at[ep],
                send_sem=ret_ssem.at[0],
                recv_sem=ret_rsem.at[0],
                device_id=(peer, tp),
                device_id_type=MESH,
            ).start()

        @pl.when(peer == ep)
        def _():
            pltpu.make_async_copy(ret_send.at[ep], ret_recv.at[ep], ret_rsem.at[0]).start()

    def contract(b):
        if b == 0:
            loads["wd"].wait()
        order = [(offset, c) for offset in range(min(2, n_tp)) for c in range(chunks)]
        order += [(offset, c) for c in range(chunks) for offset in range(2, n_tp)]
        total = None
        for offset, c in order:
            source = tp_source(offset)
            if offset:
                hid_copies[b, c, offset].wait_recv()
                block = hid_recv[source, b, c]
            else:
                block = hid_send[b, c]
            start = pl.multiple_of(source * (chunk * chunks) + c * chunk, LANES)
            term = dot(block, wd[pl.ds(start, chunk), :])
            total = term if total is None else total + term
        for e in range(span_ep):
            ret_send[b * span_ep + e] = total[e * rows : (e + 1) * rows, :].astype(BF16)
        each(span_ep, lambda step: ret_copy(b, step))

    for b in range(batches):
        expand(b)
    for b in range(batches):
        contract(b)

    row_index = lax.broadcasted_iota(jnp.int32, (rows, 1), 0)
    per_group = n_ep // GROUPS
    ids, shares = [], []
    for j in range(TOP):
        picked = jnp.zeros((rows, 1), jnp.int32)
        share = jnp.zeros((rows, 1), F32)
        for s in range(rows):
            picked = jnp.where(
                row_index == s, route_group[s] * per_group + route_expert[j, s], picked
            )
            share = jnp.where(row_index == s, route_weight[j, s], share)
        ids.append(picked)
        shares.append(share)
    for copy in q_copies + att_copies + list(hid_copies.values()):
        copy.wait_send()
    for y_off in range(pairs):
        block = mix_recv.at[0, pl.ds(0, n_ep - 1)]
        pltpu.make_async_copy(block, block, mix_ssem.at[y_off]).wait()
    for copy in near_copies[1:]:
        copy.wait_send()

    @pl.when(core == 0)
    def _():
        near_copies[0].wait_send()

    @pl.when(core == 1)
    def _():
        for b in range(batches):
            for k in range(n_tp):
                relay_copy(k, b).wait_send()

    pltpu.make_async_copy(ret_recv, ret_recv, ret_rsem.at[0]).wait()
    moe = None
    for picked, share in zip(ids, shares):
        result = jnp.zeros((rows, width), F32)
        for e in range(n_ep):
            result = jnp.where(picked == e, ret_recv[e].astype(F32), result)
        moe = share * result if moe is None else moe + share * result
    out[...] = (mix_send[...].astype(F32) + moe).astype(BF16)
    block = ret_recv.at[pl.ds(0, n_ep - 1)]
    pltpu.make_async_copy(block, block, ret_ssem.at[0]).wait()


def on_device(
    tokens,
    attn_gain,
    ffn_gain,
    w_query,
    w_key,
    w_value,
    w_forget,
    forget_bias,
    w_out,
    cache_keys,
    cache_values,
    cache_logcum,
    cache_len,
    route_group,
    route_expert,
    route_weight,
    w_gate,
    w_up,
    w_down,
):
    n_ep, n_tp = lax.axis_size("ep"), lax.axis_size("tp")
    rows, depth = tokens.shape
    width = w_out.shape[1]
    part = w_gate.shape[2]
    chunk = min(part, 256)
    batches = 2 if n_ep % 2 == 0 else 1
    chunks = part // chunk
    every = n_ep * rows
    kv_width = KV_HEADS * HEAD
    hbm = pl.BlockSpec(memory_space=pl.ANY)
    small = (
        tokens,
        attn_gain.reshape(-1, LANES),
        ffn_gain.reshape(-1, LANES),
        forget_bias.reshape(1, QUERY_HEAD_COUNT),
    )
    scalars = (cache_len.reshape(1, 1), route_group, route_expert.T, route_weight.T)
    staged = (
        w_query,
        w_key,
        w_value,
        w_forget.T,
        w_out,
        cache_keys,
        cache_values,
        cache_logcum,
        w_gate,
        w_up,
        w_down,
    )
    dma = pltpu.SemaphoreType.DMA
    return pl.pallas_call(
        functools.partial(kernel, n_ep, n_tp),
        out_shape=pltpu.VMEM((rows, width), BF16),
        in_specs=[hbm] * (len(small) + len(scalars) + len(staged)),
        out_specs=pl.BlockSpec(memory_space=pltpu.VMEM),
        scratch_shapes=[pltpu.VMEM(a.shape, a.dtype) for a in small]
        + [pltpu.SMEM(a.shape, a.dtype) for a in scalars]
        + [pltpu.VMEM(a.shape[-2:], a.dtype) for a in staged]
        + [
            pltpu.VMEM((rows, 1, w_query.shape[1]), F32),
            pltpu.VMEM((n_tp, 1, w_query.shape[1]), F32),
            pltpu.VMEM((PER_KV, kv_width), BF16),
            pltpu.VMEM((n_tp, PER_KV, kv_width), BF16),
            pltpu.VMEM((kv_width // LANES, n_tp * PER_KV, LANES), F32),
            pltpu.VMEM((rows, width), BF16),
            pltpu.VMEM((n_tp, n_ep, rows, width), BF16),
            pltpu.VMEM((batches, chunks, every // batches, chunk), BF16),
            pltpu.VMEM((n_tp, batches, chunks, every // batches, chunk), BF16),
            pltpu.VMEM((n_ep, rows, width), BF16),
            pltpu.VMEM((n_ep, rows, width), BF16),
            dma((len(small) + len(scalars) + len(staged) + Q_PARTS - 1,)),
            dma((n_tp,)),
            dma((n_tp,)),
            dma((n_tp,)),
            dma((n_tp,)),
            dma((n_tp,)),
            dma((n_tp, batches)),
            dma((n_tp, batches)),
            dma((batches, chunks, n_tp)),
            dma((batches, chunks, n_tp)),
            dma((1,)),
            dma((1,)),
            pltpu.SemaphoreType.REGULAR((2,)),
            pltpu.VMEM((n_tp, 1, width), F32),
        ],
        compiler_params=pltpu.CompilerParams(
            collective_id=0, has_side_effects=True, vmem_limit_bytes=60 * 1024 * 1024
        ),
    )(
        *small,
        *scalars,
        *staged,
    )


def solution(mesh):
    placed = (
        P("ep", None),
        P(),
        P(),
        P(None, "tp"),
        P(),
        P(),
        P(),
        P(),
        P(None, "tp"),
        P(("ep", "tp"), None, None),
        P(("ep", "tp"), None, None),
        P(("ep", "tp"), None, None),
        P(("ep", "tp")),
        P("ep"),
        P("ep", None),
        P("ep", None),
        P("ep", None, "tp"),
        P("ep", None, "tp"),
        P("ep", None, "tp"),
    )
    return jax.shard_map(
        on_device, mesh=mesh, in_specs=placed, out_specs=P("ep", "tp"), check_vma=False
    )
```

```python
import functools

import jax
import jax.numpy as jnp
from jax import lax
from jax.experimental import pallas as pl
from jax.experimental.pallas import tpu as pltpu
from jax.sharding import PartitionSpec as P

QUERY_HEAD_COUNT = 32
KV_HEADS = 4
HEAD = 64
GROUPS = 4
TOP = 2
PER_KV = QUERY_HEAD_COUNT // KV_HEADS
LANES = 128
Q_PARTS = 4
SCORE_PARTS = 4
NORM_EPSILON = 1e-06
MASKED_SCORE = -1e30
F32 = jnp.float32
BF16 = jnp.bfloat16
MESH = pl.DeviceIdType.MESH


def dot(a, b):
    return jnp.dot(a, b, preferred_element_type=F32)


def as_row(ref):
    block = ref[...].astype(F32)
    return jnp.concatenate([block[i : i + 1] for i in range(block.shape[0])], axis=1)


def each(count, body):
    if count <= 8:
        for step in range(count):
            body(step)
    else:

        @pl.loop(0, count)
        def _(step):
            body(step)


def kernel(
    n_ep,
    n_tp,
    tokens_hbm,
    attn_gain_hbm,
    ffn_gain_hbm,
    forget_bias_hbm,
    cache_len_hbm,
    route_group_hbm,
    route_expert_hbm,
    route_weight_hbm,
    wq_hbm,
    wk_hbm,
    wv_hbm,
    wf_hbm,
    wo_hbm,
    keys_hbm,
    values_hbm,
    logcum_hbm,
    wg_hbm,
    wu_hbm,
    wd_hbm,
    out,
    tokens,
    attn_gain,
    ffn_gain,
    forget_bias,
    cache_len,
    route_group,
    route_expert,
    route_weight,
    wq,
    wk,
    wv,
    wf,
    wo,
    keys,
    values,
    logcum,
    wg,
    wu,
    wd,
    q_send,
    q_recv,
    att_send,
    att_recv,
    att_rows,
    mix_send,
    mix_recv,
    hid_send,
    hid_recv,
    ret_send,
    ret_recv,
    load_sem,
    send_sem,
    q_rsem,
    att_rsem,
    mix_rsem,
    hid_rsem,
    ret_rsem,
    near_sem,
    gain_parts,
):
    ep = lax.axis_index("ep")
    tp = lax.axis_index("tp")
    pairs = n_tp // 2

    def tp_peer(offset):
        pair = lax.rem(tp // 2 + offset // 2, pairs)
        core = lax.rem(lax.rem(tp, 2) + offset % 2, 2)
        return pair * 2 + core

    def tp_source(offset):
        pair = lax.rem(tp // 2 + pairs - offset // 2, pairs)
        core = lax.rem(lax.rem(tp, 2) + offset % 2, 2)
        return pair * 2 + core

    def ep_peer(offset):
        return lax.rem(ep + offset, n_ep)

    def far_first(step, skip):
        return skip + lax.rem(step + n_ep // 2 - 2 * skip, n_ep - skip)

    q_part = wq.shape[0] // Q_PARTS
    q_names = [f"wq{i}" for i in range(Q_PARTS)]
    small = ("ffn_gain", "forget_bias", "cache_len", "route_group", "route_expert", "route_weight")
    groups = (
        ("tokens", "attn_gain"),
        *[(name,) for name in q_names],
        ("wk",),
        ("wv", "wf", *small, "logcum"),
        ("keys", "values"),
        ("wo", "wg", "wu", "wd"),
    )
    pieces = {
        "tokens": (tokens_hbm, tokens),
        "attn_gain": (attn_gain_hbm, attn_gain),
        "ffn_gain": (ffn_gain_hbm, ffn_gain),
        "forget_bias": (forget_bias_hbm, forget_bias),
        "cache_len": (cache_len_hbm, cache_len),
        "route_group": (route_group_hbm, route_group),
        "route_expert": (route_expert_hbm, route_expert),
        "route_weight": (route_weight_hbm, route_weight),
        "wk": (wk_hbm, wk),
        "wv": (wv_hbm, wv),
        "wf": (wf_hbm, wf),
        "logcum": (logcum_hbm.at[0], logcum),
        "keys": (keys_hbm.at[0], keys),
        "values": (values_hbm.at[0], values),
        "wo": (wo_hbm, wo),
        "wg": (wg_hbm.at[0], wg),
        "wu": (wu_hbm.at[0], wu),
        "wd": (wd_hbm.at[0], wd),
    }
    for i, name in enumerate(q_names):
        part = pl.ds(i * q_part, q_part)
        pieces[name] = (wq_hbm.at[part], wq.at[part])
    loads = {
        name: pltpu.make_async_copy(*pieces[name], load_sem.at[index])
        for index, names in enumerate(groups)
        for name in names
    }

    def loaded(first):
        for names in groups:
            if names[0] == first:
                for name in names:
                    loads[name].wait()

    def drain(block, sem):
        pltpu.make_async_copy(block, block, sem).wait()

    for name in ("tokens", "attn_gain", *q_names):
        loads[name].start()

    barrier = pltpu.get_barrier_semaphore()
    leader = n_tp - 1
    for offset in range(1, n_tp):
        pl.semaphore_signal(barrier, inc=1, device_id=(ep, tp_peer(offset)), device_id_type=MESH)
    for names in groups[1 + Q_PARTS :]:
        for name in names:
            loads[name].start()

    rows = tokens.shape[0]
    width = wo.shape[1]
    depth = tokens.shape[1]
    length = keys.shape[0]
    loaded("tokens")
    stream = tokens[...].astype(F32)
    square = jnp.mean(stream * stream, axis=-1, keepdims=True)
    normed = (stream * lax.rsqrt(square + NORM_EPSILON) * as_row(attn_gain)).astype(BF16)

    query = None
    for i, name in enumerate(q_names):
        loads[name].wait()
        term = dot(normed[:, i * q_part : (i + 1) * q_part], wq[i * q_part : (i + 1) * q_part, :])
        query = term if query is None else query + term
    query = query.astype(BF16).astype(F32)
    for row in range(rows):
        q_send[row] = query[row : row + 1, :]

    @pl.when(tp != leader)
    def _():
        pl.semaphore_wait(barrier, n_tp - 1)
        pl.semaphore_signal(near_sem.at[0], inc=1, device_id=(ep, leader), device_id_type=MESH)

    @pl.when(tp == leader)
    def _():
        pl.semaphore_wait(near_sem.at[0], n_tp - 1)

        def announce(step):
            pl.semaphore_signal(
                barrier, inc=1, device_id=(ep_peer(step + 1), leader), device_id_type=MESH
            )

        each(n_ep - 1, announce)

    core = lax.rem(tp, 2)
    pair = tp // 2
    partner = tp + 1 - 2 * core

    def far_pair(p):
        return lax.rem(pair + p, pairs) * 2

    peers = [far_pair(p) + d for p in range(1, pairs) for d in (0, 1)] + [partner]

    def to_peer(source, target, peer, arrived):
        return pltpu.make_async_remote_copy(
            src_ref=source,
            dst_ref=target,
            send_sem=send_sem.at[0],
            recv_sem=arrived,
            device_id=(ep, peer),
            device_id_type=MESH,
        )

    for peer in peers:
        to_peer(q_send.at[peer], q_recv.at[tp], peer, q_rsem.at[0]).start()
    pltpu.make_async_copy(q_send.at[tp], q_recv.at[tp], q_rsem.at[0]).start()

    own = lax.broadcasted_iota(jnp.int32, (rows, 1), 0) == tp

    def own_row(values_all):
        return jnp.sum(jnp.where(own, values_all, 0.0), axis=0, keepdims=True)

    loaded("wk")
    key_new = own_row(dot(normed, wk[...])).astype(BF16).astype(F32)
    loaded("wv")
    value_new = own_row(dot(normed, wv[...])).astype(BF16).astype(F32)
    heads = QUERY_HEAD_COUNT
    gates = lax.dot_general(
        wf[...], normed, (((1,), (1,)), ((), ())), preferred_element_type=F32
    )
    own_lane = lax.broadcasted_iota(jnp.int32, (1, rows), 1) == tp
    gate_sum = jnp.sum(jnp.where(own_lane, gates, 0.0), axis=1, keepdims=True)
    diagonal = lax.broadcasted_iota(jnp.int32, (heads, heads), 0) == lax.broadcasted_iota(
        jnp.int32, (heads, heads), 1
    )
    bias_sum = jnp.sum(jnp.where(diagonal, forget_bias[...], 0.0), axis=1, keepdims=True)
    log_gate = jax.nn.log_sigmoid(gate_sum + bias_sum)
    used = cache_len[0, 0]
    position = lax.broadcasted_iota(jnp.int32, (1, length), 1)
    cum = logcum[...]
    latest = jnp.sum(jnp.where(position == used - 1, cum, 0.0), axis=1, keepdims=True)
    bias = jnp.where(position < used, (latest + log_gate) - cum, MASKED_SCORE)

    loaded("keys")
    drain(q_recv, q_rsem.at[0])

    span = PER_KV * HEAD
    q_row = jnp.concatenate([q_recv[source] for source in range(n_tp)], axis=1)
    row_of = lax.broadcasted_iota(jnp.int32, (PER_KV, span), 0)
    lane_of = lax.broadcasted_iota(jnp.int32, (PER_KV, span), 1) // HEAD
    half_of = lax.broadcasted_iota(jnp.int32, (PER_KV, LANES), 1) // HEAD
    zeros = jnp.zeros((PER_KV, LANES), F32)
    blocks = []
    for head in range(KV_HEADS):
        part = jnp.broadcast_to(q_row[:, head * span : (head + 1) * span], (PER_KV, span))
        part = jnp.where(row_of == lane_of, part, 0.0)
        fold = part[:, :LANES]
        for tile in range(1, span // LANES):
            fold = fold + part[:, tile * LANES : (tile + 1) * LANES]
        fold = fold + pltpu.roll(fold, HEAD, 1)
        fold = jnp.where(half_of == head % 2, fold, 0.0)
        tiles = [zeros] * (KV_HEADS * HEAD // LANES)
        tiles[head * HEAD // LANES] = fold
        blocks.append(jnp.concatenate(tiles, axis=1))
    q_heads = jnp.concatenate(blocks, axis=0) * HEAD ** (-0.5)
    own_score = jnp.sum(q_heads * key_new, axis=1, keepdims=True)
    q_heads = q_heads.astype(BF16)
    block = length // SCORE_PARTS
    parts = []
    for i in range(SCORE_PARTS):
        used_rows = slice(i * block, (i + 1) * block)
        score = lax.dot_general(
            q_heads, keys[used_rows, :], (((1,), (1,)), ((), ())), preferred_element_type=F32
        )
        score = score + bias[:, used_rows]
        top = jnp.max(score, axis=1, keepdims=True)
        weight = jnp.exp(score - top)
        total = jnp.sum(weight, axis=1, keepdims=True)
        parts.append((top, total, dot(weight.astype(BF16), values[used_rows, :])))
    peak = own_score
    for top, _, _ in parts:
        peak = jnp.maximum(peak, top)
    own_weight = jnp.exp(own_score - peak)
    denominator = own_weight
    summed = own_weight.astype(BF16).astype(F32) * value_new
    for top, total, product in parts:
        share = jnp.exp(top - peak)
        denominator = denominator + share * total
        summed = summed + share * product
    summed = summed / denominator
    kv_of = lax.broadcasted_iota(jnp.int32, (PER_KV, KV_HEADS * HEAD), 1) // HEAD
    folded = summed[:PER_KV]
    for head in range(1, KV_HEADS):
        folded = jnp.where(kv_of == head, summed[head * PER_KV : (head + 1) * PER_KV], folded)
    attended = folded.astype(BF16)
    att_send[...] = attended

    for peer in peers:
        to_peer(att_send, att_recv.at[tp], peer, att_rsem.at[0]).start()
    pltpu.make_async_copy(att_send, att_recv.at[tp], att_rsem.at[0]).start()
    loaded("wo")

    @pl.when(tp == leader)
    def _():
        pl.semaphore_wait(barrier, n_tp + n_ep - 2)
        for offset in range(1, n_tp):
            pl.semaphore_signal(
                near_sem.at[1], inc=1, device_id=(ep, tp_peer(offset)), device_id_type=MESH
            )

    gain = as_row(ffn_gain)
    for source in range(n_tp):
        gain_parts[source] = gain[:, source * width : (source + 1) * width]
    drain(att_recv, att_rsem.at[0])
    for source in range(n_tp):
        arrived = att_recv[source].astype(F32)
        for tile in range(att_rows.shape[0]):
            att_rows[tile, source * PER_KV : (source + 1) * PER_KV] = arrived[
                :, tile * LANES : (tile + 1) * LANES
            ]
    left = jnp.concatenate(
        [
            att_rows[tile, pl.ds(j, n_tp, stride=PER_KV), :]
            for j in range(PER_KV)
            for tile in range(att_rows.shape[0])
        ],
        axis=1,
    ).astype(BF16)
    right = jnp.concatenate(
        [
            wo[head * span + j * HEAD : head * span + (j + 1) * HEAD, :]
            for j in range(PER_KV)
            for head in range(KV_HEADS)
        ],
        axis=0,
    )
    projected = dot(left, right)
    residual = tokens[:, pl.ds(pl.multiple_of(tp * width, LANES), width)].astype(F32)
    mixed = (residual + projected).astype(BF16)
    mix_send[...] = mixed

    @pl.when(tp != leader)
    def _():
        pl.semaphore_wait(near_sem.at[1], 1)

    batches, chunks, _, _, chunk = hid_recv.shape
    span_ep = n_ep // batches
    batch = ep // span_ep
    home = mix_recv.at[core, pair, ep]
    home_sem = mix_rsem.at[core, batch]

    def mix_copy(step, y_off):
        return pltpu.make_async_remote_copy(
            src_ref=mix_send,
            dst_ref=home,
            send_sem=send_sem.at[0],
            recv_sem=home_sem,
            device_id=(ep_peer(step), far_pair(y_off) + 1),
            device_id_type=MESH,
        )

    for y_off in range(pairs - 1, -1, -1):
        each(n_ep - 1, lambda step, y_off=y_off: mix_copy(far_first(step, 1), y_off).start())
    for y_off in range(1, pairs):
        mix_copy(0, y_off).start()

    @pl.when(core == 0)
    def _():
        mix_copy(0, 0).start()

    @pl.when(core == 1)
    def _():
        pltpu.make_async_copy(mix_send, home, home_sem).start()

    def mix_block(side, b):
        return mix_recv.at[side, :, pl.ds(b * span_ep, span_ep)]


    def expand(b):
        gates, ups = [None] * chunks, [None] * chunks
        square = None

        @pl.when(core == 1)
        def _():
            for side in (1, 0):
                block = mix_block(side, b)
                drain(block, mix_rsem.at[side, b])
                to_peer(block, block, partner, mix_rsem.at[side, b]).start()

        for k in range(n_tp):
            side, line = 1 - k // pairs, lax.rem(pair + k % pairs, pairs)
            if k % pairs == 0:
                @pl.when(core == 0)
                def _(side=side):
                    drain(mix_block(side, b), mix_rsem.at[side, b])

            source = line * 2 + side
            wide = jnp.concatenate(
                [mix_recv[side, line, b * span_ep + e].astype(F32) for e in range(span_ep)], axis=0
            )
            term = jnp.sum(wide * wide, axis=-1, keepdims=True)
            square = term if square is None else square + term
            scaled = (wide * gain_parts[source]).astype(BF16)
            start = pl.multiple_of(source * width, LANES)
            for c in range(chunks):
                cols = slice(c * chunk, (c + 1) * chunk)
                gate = dot(scaled, wg[pl.ds(start, width), cols])
                up = dot(scaled, wu[pl.ds(start, width), cols])
                gates[c] = gate if k == 0 else gates[c] + gate
                ups[c] = up if k == 0 else ups[c] + up
        factor = lax.rsqrt(square * (1.0 / depth) + NORM_EPSILON)
        for c in range(chunks):
            gate = gates[c] * factor
            hidden = (gate / (1.0 + jnp.exp(-gate)) * (ups[c] * factor)).astype(BF16)
            hid_send[b, c] = hidden
            for peer in peers:
                arrived = hid_rsem.at[b, 0 if peer is partner else 1 + c]
                to_peer(hid_send.at[b, c], hid_recv.at[b, c, tp], peer, arrived).start()

    def ret_copy(b, step):
        peer = b * span_ep + lax.rem(ep + span_ep // 2 + step, span_ep)

        @pl.when(peer != ep)
        def _():
            pltpu.make_async_remote_copy(
                src_ref=ret_send.at[peer],
                dst_ref=ret_recv.at[ep],
                send_sem=send_sem.at[1],
                recv_sem=ret_rsem.at[0],
                device_id=(peer, tp),
                device_id_type=MESH,
            ).start()

        @pl.when(peer == ep)
        def _():
            pltpu.make_async_copy(ret_send.at[ep], ret_recv.at[ep], ret_rsem.at[0]).start()

    def contract(b):
        total = None

        def add(source, c, block):
            nonlocal total
            start = pl.multiple_of(source * (chunk * chunks) + c * chunk, LANES)
            term = dot(block, wd[pl.ds(start, chunk), :])
            total = term if total is None else total + term

        for c in range(chunks):
            add(tp, c, hid_send[b, c])
        drain(hid_recv.at[b, :, partner], hid_rsem.at[b, 0])
        for c in range(chunks):
            add(partner, c, hid_recv[b, c, partner])
        for c in range(chunks):
            drain(hid_recv.at[b, c, pl.ds(0, n_tp - 2)], hid_rsem.at[b, 1 + c])
            for p in range(1, pairs):
                for d in (1, 0):
                    add(far_pair(p) + d, c, hid_recv[b, c, far_pair(p) + d])
        for e in range(span_ep):
            ret_send[b * span_ep + e] = total[e * rows : (e + 1) * rows, :].astype(BF16)
        each(span_ep, lambda step: ret_copy(b, step))

    for b in range(batches):
        expand(b)
    for b in range(batches):
        contract(b)

    row_index = lax.broadcasted_iota(jnp.int32, (rows, 1), 0)
    per_group = n_ep // GROUPS
    ids, shares = [], []
    for j in range(TOP):
        picked = jnp.zeros((rows, 1), jnp.int32)
        share = jnp.zeros((rows, 1), F32)
        for s in range(rows):
            picked = jnp.where(
                row_index == s, route_group[s] * per_group + route_expert[j, s], picked
            )
            share = jnp.where(row_index == s, route_weight[j, s], share)
        ids.append(picked)
        shares.append(share)
    drain(q_recv.at[pl.ds(0, n_tp - 1)], send_sem.at[0])
    drain(att_recv.at[pl.ds(0, n_tp - 1)], send_sem.at[0])
    drain(mix_recv.at[0, :, pl.ds(0, n_ep - 1)], send_sem.at[0])
    drain(mix_recv.at[0, pl.ds(0, pairs - 1), 0], send_sem.at[0])
    drain(hid_recv.at[:, :, pl.ds(0, n_tp - 1)], send_sem.at[0])

    @pl.when(core == 0)
    def _():
        drain(mix_recv.at[0, 0, 0], send_sem.at[0])

    @pl.when(core == 1)
    def _():
        drain(mix_recv, send_sem.at[0])

    drain(ret_recv, ret_rsem.at[0])
    moe = None
    for picked, share in zip(ids, shares):
        result = jnp.zeros((rows, width), F32)
        for e in range(n_ep):
            result = jnp.where(picked == e, ret_recv[e].astype(F32), result)
        moe = share * result if moe is None else moe + share * result
    out[...] = (mix_send[...].astype(F32) + moe).astype(BF16)
    drain(ret_recv.at[pl.ds(0, n_ep - 1)], send_sem.at[1])


def on_device(
    tokens,
    attn_gain,
    ffn_gain,
    w_query,
    w_key,
    w_value,
    w_forget,
    forget_bias,
    w_out,
    cache_keys,
    cache_values,
    cache_logcum,
    cache_len,
    route_group,
    route_expert,
    route_weight,
    w_gate,
    w_up,
    w_down,
):
    n_ep, n_tp = lax.axis_size("ep"), lax.axis_size("tp")
    rows, depth = tokens.shape
    width = w_out.shape[1]
    part = w_gate.shape[2]
    chunk = min(part, 256)
    batches = 2 if n_ep % 2 == 0 else 1
    chunks = part // chunk
    every = n_ep * rows
    kv_width = KV_HEADS * HEAD
    hbm = pl.BlockSpec(memory_space=pl.ANY)
    small = (
        tokens,
        attn_gain.reshape(-1, LANES),
        ffn_gain.reshape(-1, LANES),
        forget_bias.reshape(1, QUERY_HEAD_COUNT),
    )
    scalars = (cache_len.reshape(1, 1), route_group, route_expert.T, route_weight.T)
    staged = (
        w_query,
        w_key,
        w_value,
        w_forget.T,
        w_out,
        cache_keys,
        cache_values,
        cache_logcum,
        w_gate,
        w_up,
        w_down,
    )
    dma = pltpu.SemaphoreType.DMA
    return pl.pallas_call(
        functools.partial(kernel, n_ep, n_tp),
        out_shape=pltpu.VMEM((rows, width), BF16),
        in_specs=[hbm] * (len(small) + len(scalars) + len(staged)),
        out_specs=pl.BlockSpec(memory_space=pltpu.VMEM),
        scratch_shapes=[pltpu.VMEM(a.shape, a.dtype) for a in small]
        + [pltpu.SMEM(a.shape, a.dtype) for a in scalars]
        + [pltpu.VMEM(a.shape[-2:], a.dtype) for a in staged]
        + [
            pltpu.VMEM((rows, 1, w_query.shape[1]), F32),
            pltpu.VMEM((n_tp, 1, w_query.shape[1]), F32),
            pltpu.VMEM((PER_KV, kv_width), BF16),
            pltpu.VMEM((n_tp, PER_KV, kv_width), BF16),
            pltpu.VMEM((kv_width // LANES, n_tp * PER_KV, LANES), F32),
            pltpu.VMEM((rows, width), BF16),
            pltpu.VMEM((2, n_tp // 2, n_ep, rows, width), BF16),
            pltpu.VMEM((batches, chunks, every // batches, chunk), BF16),
            pltpu.VMEM((batches, chunks, n_tp, every // batches, chunk), BF16),
            pltpu.VMEM((n_ep, rows, width), BF16),
            pltpu.VMEM((n_ep, rows, width), BF16),
            dma((5 + Q_PARTS,)),
            dma((2,)),
            dma((1,)),
            dma((1,)),
            dma((2, batches)),
            dma((batches, 1 + chunks)),
            dma((1,)),
            pltpu.SemaphoreType.REGULAR((2,)),
            pltpu.VMEM((n_tp, 1, width), F32),
        ],
        compiler_params=pltpu.CompilerParams(
            collective_id=0, has_side_effects=True, vmem_limit_bytes=60 * 1024 * 1024
        ),
    )(
        *small,
        *scalars,
        *staged,
    )


def solution(mesh):
    placed = (
        P("ep", None),
        P(),
        P(),
        P(None, "tp"),
        P(),
        P(),
        P(),
        P(),
        P(None, "tp"),
        P(("ep", "tp"), None, None),
        P(("ep", "tp"), None, None),
        P(("ep", "tp"), None, None),
        P(("ep", "tp")),
        P("ep"),
        P("ep", None),
        P("ep", None),
        P("ep", None, "tp"),
        P("ep", None, "tp"),
        P("ep", None, "tp"),
    )
    return jax.shard_map(
        on_device, mesh=mesh, in_specs=placed, out_specs=P("ep", "tp"), check_vma=False
    )
```
